32 devices in a mesh: ep: 4 (over y, x), tp: 8 (over z, core).
Axes of the slice: x: 2, y: 2, z: 4, core: 2. Of those that a mesh axis runs over, the one named last changes fastest.
Arguments:
- mix_tokens: bfloat16 [4096, 2048], P(('ep', 'tp')), may hold values from -6 to 6
- mix_gain: bfloat16 [2048], replicated, may hold values from 0.099609375 to 1.8984375
- gate_proj: bfloat16 [2048, 1024], P(None, 'tp'), may hold values from -0.125 to 0.125
- conv_proj: bfloat16 [2048, 1024], P(None, 'tp'), may hold values from -0.125 to 0.125
- value_proj: bfloat16 [2048, 1024], P(None, 'tp'), may hold values from -0.125 to 0.125
- conv_taps: bfloat16 [3, 1024], P(None, 'tp'), may hold values from -3 to 3
- out_proj: bfloat16 [1024, 2048], P('tp'), may hold values from -0.1875 to 0.1875
- moe_tokens: bfloat16 [2048, 2048], P(('ep', 'tp')), may hold values from -6 to 6
- moe_gain: bfloat16 [2048], replicated, may hold values from 0.099609375 to 1.8984375
- expert_ids: int32 [2048, 2], P(('ep', 'tp')), may hold values from 0 to 3, all different within a row; in each aligned block of 64 rows (0 to 63, 64 to 127, ...) at most 36 rows name the same one
- expert_scores: float32 [2048, 2], P(('ep', 'tp')), may hold values from -6 to 6
- expert_gate: bfloat16 [4, 2048, 4096], P('ep', None, 'tp'), may hold values from -0.125 to 0.125
- expert_up: bfloat16 [4, 2048, 4096], P('ep', None, 'tp'), may hold values from -0.125 to 0.125
- expert_down: bfloat16 [4, 4096, 2048], P('ep', 'tp'), may hold values from -0.09375 to 0.09375
Outputs:
- mix_out: bfloat16 [4096, 2048], P(('ep', 'tp'))
- moe_out: bfloat16 [2048, 2048], P(('ep', 'tp'))
The draws below stay inside these ranges and needn't reach their ends.
Inputs may be any that keep to these rules, and one draw needn't show every extreme that they name: `expert_ids`: each row names 2 different experts; among the rows of one device no expert is named more than 36 times.
All inputs are finite; a program needn't handle non-finite values.
Results may differ from the reference program's by a relative error of at most 0.018.
Values may be sent and summed in bfloat16 or wider, within the bound.
A program may use at most 128 MiB of HBM per device.

```python
import math
import jax
import jax.numpy as jnp
import numpy as np
from jax import lax

D = 2048
CONV = 1024
FF = 4096
TAPS = 3
TOP = 2
MOE_DEV = 64
EXPERTS = 4
CAP = 36
MIX_TOKENS = 4096
MOE_TOKENS = 2048
N_EP = 4
N_TP = 8


def shard_levels(own_key, dims, shards, low, high):
    gain, own = 1.0, jax.random.fold_in(own_key, 6)
    for dim, blocks in shards:
        draws = jnp.exp(jax.random.uniform(jax.random.fold_in(own, dim), (blocks,), jnp.float32, low / len(shards), high / len(shards)))
        gain = gain * jnp.repeat(draws, dims[dim] // blocks).reshape([-1 if axis == dim else 1 for axis in range(len(dims))])
    return gain


def deal_out(key, own, number, rows, count, top, most, lean):
    order = jax.random.permutation(key, count)
    crowded, ordinary = shares(count, rows * top, most, lean, True), shares(count, rows * top, most, lean, False)
    places = jnp.arange(count)

    def named(tallies, rotation):
        used = int((tallies > 0).sum())
        fixed = max(1, used // 4)
        shifted = fixed + (places - fixed + rotation * (used - fixed)) % max(1, count - fixed)
        return jnp.zeros((count,), jnp.int32).at[order[jnp.where(places < fixed, places, shifted)]].set(jnp.asarray(tallies, jnp.int32))

    tallies = jnp.where(number % 4 == 0, named(crowded, number // 4), named(ordinary, number - number // 4 - 1))
    mixed = jax.random.permutation(jax.random.fold_in(own, 3), count)
    donor, taker = mixed[0:count // 2 * 2:2], mixed[1:count // 2 * 2:2]
    room = jnp.minimum(tallies[donor] - 1, most - tallies[taker]) // 2
    room = jnp.where((donor == order[0]) | (taker == order[0]) | (tallies[taker] == 0), 0, jnp.maximum(room, 0))
    shifted = jax.random.randint(jax.random.fold_in(own, 4), (count // 2,), 0, 1 << 20) % (room + 1)
    tallies = tallies.at[donor].add(-shifted).at[taker].add(shifted)
    labels = jnp.searchsorted(jnp.cumsum(tallies), jnp.arange(rows * top), side="right").astype(jnp.int32)
    listing = labels.reshape(top, rows).T
    listing = listing[jax.random.permutation(jax.random.fold_in(own, 1), rows)]
    rotation = jax.random.randint(jax.random.fold_in(own, 2), (rows, 1), 0, top)
    return jnp.take_along_axis(listing, (jnp.arange(top)[None, :] + rotation) % top, axis=1)


def shares(number_of, total, most, slope, full):
    loads = [(1 << 20) // math.isqrt(standing ** slope) + 1 for standing in range(1, number_of + 1)]
    largest = most if full else min(most, max(-(-total // number_of), total * loads[0] // sum(loads)))
    least = 1 if total - largest >= number_of - 1 else 0
    given, surplus = [largest] + [least] * (number_of - 1), total - largest - least * (number_of - 1)
    while surplus > 0:
        candidates = [i for i in range(1, number_of) if given[i] < largest] or [i for i in range(1, number_of) if given[i] < most]
        mass, budget = sum([loads[i] for i in candidates]), surplus
        for i in candidates:
            addition = min(most - given[i], max(1, budget * loads[i] // mass), surplus)
            given[i] = given[i] + addition
            surplus = surplus - addition
    return np.array(given)


def centred(own_key, extent, spread, reach, split=(), kind=jnp.bfloat16):
    values = jax.random.normal(own_key, extent, jnp.float32) * spread
    if len(split) > 0:
        values = shard_levels(own_key, extent, split, -0.22, 0.18) * values
    return jnp.clip(values, min=-reach, max=reach).astype(kind)


def setup_inputs(seed: int = 0) -> dict:
    keys = jax.random.split(jax.random.key(seed), 15)
    mix_tokens = centred(keys[0], (MIX_TOKENS, D), 1.0, 6.0, ((0, 32),))
    mix_gain = jnp.clip(1.0 + 0.18 * jax.random.normal(keys[1], (D,), jnp.float32), 0.099609375, 1.8984375).astype(jnp.bfloat16)
    gate_proj = centred(keys[2], (D, CONV), D ** -0.5, 0.125, ((1, 8),))
    conv_proj = centred(keys[3], (D, CONV), D ** -0.5, 0.125, ((1, 8),))
    value_proj = centred(keys[4], (D, CONV), D ** -0.5, 0.125, ((1, 8),))
    conv_taps = centred(keys[5], (TAPS, CONV), 0.577, 3.0, ((1, 8),))
    out_proj = centred(keys[6], (CONV, D), CONV ** -0.5, 0.1875, ((0, 8),))
    moe_tokens = centred(keys[7], (MOE_TOKENS, D), 1.0, 6.0, ((0, 32),))
    moe_gain = jnp.clip(1.0 + 0.18 * jax.random.normal(keys[8], (D,), jnp.float32), 0.099609375, 1.8984375).astype(jnp.bfloat16)
    expert_ids_keys = jax.random.split(jax.random.fold_in(keys[9], 1), MOE_TOKENS // MOE_DEV)
    expert_ids_turns = jax.random.permutation(jax.random.fold_in(keys[9], 3), MOE_TOKENS // MOE_DEV)
    expert_ids = jax.vmap(lambda own, number: deal_out(jax.random.fold_in(keys[9], 2), own, number, MOE_DEV, EXPERTS, TOP, CAP, 2))(expert_ids_keys, expert_ids_turns).reshape((MOE_TOKENS, TOP))
    expert_scores = centred(keys[10], (MOE_TOKENS, TOP), 1.0, 6.0, ((0, 32),), jnp.float32)
    expert_gate = centred(keys[11], (EXPERTS, D, FF), D ** -0.5, 0.125, ((0, 4), (2, 8)))
    expert_up = centred(keys[12], (EXPERTS, D, FF), D ** -0.5, 0.125, ((0, 4), (2, 8)))
    expert_down = centred(keys[13], (EXPERTS, FF, D), FF ** -0.5, 0.09375, ((0, 4), (1, 8)))
    return {"mix_tokens": mix_tokens, "mix_gain": mix_gain, "gate_proj": gate_proj, "conv_proj": conv_proj, "value_proj": value_proj, "conv_taps": conv_taps, "out_proj": out_proj, "moe_tokens": moe_tokens, "moe_gain": moe_gain, "expert_ids": expert_ids, "expert_scores": expert_scores, "expert_gate": expert_gate, "expert_up": expert_up, "expert_down": expert_down}


norm_eps = 1e-06

def scaled_norm(row_data, gain_vec):
    values = row_data.astype(jnp.float32)
    inverse = lax.rsqrt(lax.optimization_barrier(jnp.mean(values * values, axis=1, keepdims=True)) + norm_eps)
    return (values * inverse * gain_vec.astype(jnp.float32)).astype(jnp.bfloat16)

def reference(mix_tokens, mix_gain, gate_proj, conv_proj, value_proj, conv_taps, out_proj, moe_tokens, moe_gain, expert_ids, expert_scores, expert_gate, expert_up, expert_down):
    normed = scaled_norm(mix_tokens, mix_gain)
    out_gate = jnp.dot(normed, gate_proj, preferred_element_type=jnp.float32).astype(jnp.bfloat16)
    in_gate = jnp.dot(normed, conv_proj, preferred_element_type=jnp.float32).astype(jnp.bfloat16)
    values = jnp.dot(normed, value_proj, preferred_element_type=jnp.float32).astype(jnp.bfloat16)
    signal = (in_gate.astype(jnp.float32) * values.astype(jnp.float32)).astype(jnp.bfloat16)
    length = signal.shape[0]
    padded = jnp.concatenate([jnp.zeros((TAPS - 1, CONV), jnp.bfloat16), signal], axis=0)
    tap_values = conv_taps.astype(jnp.float32)
    convolved = jnp.zeros((length, CONV), jnp.float32)
    for offset in range(TAPS):
        convolved = convolved + padded[offset:offset + length].astype(jnp.float32) * tap_values[offset]
    carried = (out_gate.astype(jnp.float32) * convolved).astype(jnp.bfloat16)
    mix_out = jnp.dot(carried, out_proj, preferred_element_type=jnp.float32).astype(jnp.bfloat16)
    moe_normed = scaled_norm(moe_tokens, moe_gain)
    flat_ids = expert_ids.reshape(-1).astype(jnp.int32)
    assigned = flat_ids.shape[0]
    bound = N_EP * N_TP * CAP
    onehot = (flat_ids[:, None] == jnp.arange(EXPERTS, dtype=jnp.int32)[None, :]).astype(jnp.int32)
    slot_rank = lax.optimization_barrier(jnp.sum((jnp.cumsum(onehot, axis=0) - onehot) * onehot, axis=1)).astype(jnp.int32)
    owner = (jnp.arange(assigned, dtype=jnp.int32) // TOP).astype(jnp.int32)
    table = jnp.zeros((EXPERTS, bound), jnp.int32).at[flat_ids, slot_rank].set(owner)
    hidden_block = FF // N_TP

    def one_expert(expert_index):
        chosen = moe_normed[table[expert_index]]
        gate_value = jnp.dot(chosen, expert_gate[expert_index], preferred_element_type=jnp.float32)
        up_value = jnp.dot(chosen, expert_up[expert_index], preferred_element_type=jnp.float32)
        hidden = (jax.nn.silu(gate_value) * up_value).astype(jnp.bfloat16)
        down = expert_down[expert_index]

        def add_block(block_index, running):
            start = (block_index * hidden_block).astype(jnp.int32)
            part_hidden = lax.dynamic_slice_in_dim(hidden, start, hidden_block, 1)
            part_weight = lax.dynamic_slice_in_dim(down, start, hidden_block, 0)
            term = jnp.dot(part_hidden, part_weight, preferred_element_type=jnp.float32).astype(jnp.bfloat16)
            term = lax.optimization_barrier(term)
            return running + term.astype(jnp.float32)
        running = lax.fori_loop(0, N_TP, add_block, jnp.zeros((bound, D), jnp.float32))
        return running.astype(jnp.bfloat16)
    results = lax.map(one_expert, jnp.arange(EXPERTS, dtype=jnp.int32))
    picked = results[flat_ids, slot_rank].reshape(-1, TOP, D)
    route_weight = jax.nn.softmax(expert_scores.astype(jnp.float32), axis=1)
    moe_out = lax.optimization_barrier(jnp.sum(route_weight[:, :, None] * picked.astype(jnp.float32), axis=1)).astype(jnp.bfloat16)
    return (mix_out, moe_out)
```

```python
import functools
import jax
import jax.numpy as jnp
from jax import lax
from jax.experimental import pallas as pl
from jax.experimental.pallas import tpu as pltpu
from jax.sharding import PartitionSpec as P

norm_eps = 1e-06
CORES = 2
ANY = pl.BlockSpec(memory_space=pl.ANY)
VMEM = pl.BlockSpec(memory_space=pltpu.VMEM)
MESH = pl.DeviceIdType.MESH
DMA = pltpu.SemaphoreType.DMA


def from_behind(value, axis, steps):
    count = lax.axis_size(axis)
    leading, last = (max(0, -steps), min(count, count - steps))
    return lax.ppermute(value, axis, [(source, source + steps) for source in range(leading, last)])


def scaled_norm(row_data, gain_vec):
    values = row_data.astype(jnp.float32)
    inverse = lax.rsqrt(jnp.mean(values * values, axis=1, keepdims=True) + norm_eps)
    return (values * inverse * gain_vec.astype(jnp.float32)).astype(jnp.bfloat16)


class Place:
    def __init__(self, n_z, n_ep):
        self.n_z, self.n_ep = n_z, n_ep
        tp = lax.axis_index("tp")
        self.z, self.core = tp // CORES, lax.rem(tp, CORES)
        self.ep = lax.axis_index("ep")
        self.up = {"tp": lax.rem(tp + CORES, n_z * CORES)}
        self.down = {"tp": lax.rem(tp + (n_z - 1) * CORES, n_z * CORES)}
        self.other = {"tp": self.z * CORES + 1 - self.core}
        self.has_up, self.has_down = self.z < n_z - 1, self.z > 0

    def peer(self, offset):
        return {"ep": lax.rem(self.ep + offset, self.n_ep)}

    def source(self, offset):
        return lax.rem(self.ep + self.n_ep - offset, self.n_ep)


def greet(place, line, sibling, peers):
    barrier = pltpu.get_barrier_semaphore()

    def tell(where):
        pl.semaphore_signal(barrier, inc=1, device_id=where, device_id_type=MESH)

    if line:
        pl.when(place.has_up)(lambda: tell(place.up))
        pl.when(place.has_down)(lambda: tell(place.down))
    if sibling:
        tell(place.other)
    if peers:
        for offset in range(1, place.n_ep):
            tell(place.peer(offset))
    count = int(sibling) + (place.n_ep - 1 if peers else 0)
    if line:
        count = count + place.has_up.astype(jnp.int32) + place.has_down.astype(jnp.int32)
    pl.semaphore_wait(barrier, count)


def remote(source, target, send, receive, where):
    return pltpu.make_async_remote_copy(
        src_ref=source,
        dst_ref=target,
        send_sem=send,
        recv_sem=receive,
        device_id=where,
        device_id_type=MESH,
    )


class LineGather:
    def __init__(self, place, own, slot, parts, send, receive, on_arrival=None):
        self.place, self.own, self.slot, self.parts = place, own, slot, parts
        self.send, self.receive, self.on_arrival = send, receive, on_arrival
        self.pending = []

    def hop(self, way, step, part, source, z):
        where = self.place.up if way == 0 else self.place.down
        return remote(
            source,
            self.slot(z, part),
            self.send.at[way, step, part],
            self.receive.at[way, step, part],
            where,
        )

    def go(self, condition, make):
        pl.when(condition)(lambda: make().start())
        self.pending.append((condition, make))

    def begin(self):
        place = self.place
        for part in range(self.parts):
            for way, has in ((0, place.has_up), (1, place.has_down)):
                self.go(
                    has,
                    functools.partial(self.hop, way, 0, part, self.own(part), place.z),
                )

    def step(self, distance):
        place = self.place
        for part in range(self.parts):
            for way in (0, 1):
                if way == 0:
                    z, here, has = place.z - distance, place.z >= distance, place.has_up
                else:
                    z = place.z + distance
                    here, has = z < place.n_z, place.has_down
                z = lax.rem(z + place.n_z, place.n_z)
                incoming = functools.partial(
                    self.hop, way, distance - 1, part, self.own(part), z
                )
                pl.when(here)(lambda incoming=incoming: incoming().wait_recv())
                if distance < place.n_z - 1:
                    self.go(
                        here & has,
                        functools.partial(self.hop, way, distance, part, self.slot(z, part), z),
                    )
                if self.on_arrival is not None:
                    self.on_arrival(here, way, distance, part, z)

    def finish(self):
        for condition, make in self.pending:
            pl.when(condition)(lambda make=make: make().wait_send())


def token_gather_kernel(n_z, n_ep, rows_ref, meta_ref, rows_out, meta_out, sems, meta_sems, local):
    place = Place(n_z, n_ep)
    rows_here = pltpu.make_async_copy(rows_ref, rows_out.at[place.z], local.at[0])
    meta_here = pltpu.make_async_copy(meta_ref, meta_out.at[place.z], local.at[1])
    rows_here.start()
    meta_here.start()
    greet(place, True, False, False)
    half = rows_ref.shape[0] // 2
    gathers = [
        LineGather(
            place,
            lambda part: rows_ref.at[pl.ds(part * half, half)],
            lambda z, part: rows_out.at[z, pl.ds(part * half, half)],
            2,
            sems.at[0],
            sems.at[1],
        ),
        LineGather(
            place,
            lambda part: meta_ref,
            lambda z, part: meta_out.at[z],
            1,
            meta_sems.at[0],
            meta_sems.at[1],
        ),
    ]
    for gather in gathers:
        gather.begin()
    for distance in range(1, n_z):
        for gather in gathers:
            gather.step(distance)
    for gather in gathers:
        gather.finish()
    rows_here.wait()
    meta_here.wait()


def token_gather(n_z, n_ep, rows, meta):
    return pl.pallas_call(
        functools.partial(token_gather_kernel, n_z, n_ep),
        out_shape=(
            jax.ShapeDtypeStruct((n_z,) + rows.shape, rows.dtype),
            jax.ShapeDtypeStruct((n_z,) + meta.shape, meta.dtype),
        ),
        in_specs=[VMEM, VMEM],
        out_specs=(ANY, ANY),
        scratch_shapes=[DMA((2, 2, n_z, 2)), DMA((2, 2, n_z, 1)), DMA((2,))],
        compiler_params=pltpu.CompilerParams(collective_id=0, has_side_effects=True),
        name="token_gather",
    )(rows, meta)


def spread_kernel(
    n_z, n_ep, mix_ref, moe_ref, mix_out, moe_out, sems, share, cross, cross_share, local
):
    place = Place(n_z, n_ep)
    half = mix_ref.shape[0] // 2
    core = place.core
    sharing = []

    def mix_slot(z, part, which):
        return mix_out.at[z, which, pl.ds(part * half, half)]

    def share_copy(slot_here, slot_sem):
        return remote(
            slot_here, slot_here, share.at[0].at[slot_sem], share.at[1].at[slot_sem], place.other
        )

    here = [
        pltpu.make_async_copy(mix_ref, mix_out.at[place.z, core], local.at[0]),
        pltpu.make_async_copy(moe_ref.at[place.ep], moe_out.at[place.ep, core], local.at[1]),
    ]
    for copy in here:
        copy.start()
    greet(place, True, True, True)

    def on_arrival(condition, way, distance, part, z):
        sem = (way * n_z + distance) * 2 + part

        def make():
            return share_copy(mix_slot(z, part, core), sem)

        pl.when(condition)(lambda: make().start())
        sharing.append((condition, make))

    gather = LineGather(
        place,
        lambda part: mix_ref.at[pl.ds(part * half, half)],
        lambda z, part: mix_slot(z, part, core),
        2,
        sems.at[0],
        sems.at[1],
        on_arrival,
    )
    gather.begin()
    crossings = []
    for offset in range(1, n_ep):
        peer = place.peer(offset)
        copy = remote(
            moe_ref.at[peer["ep"]],
            moe_out.at[place.ep, core],
            cross.at[0, offset],
            cross.at[1, offset],
            peer,
        )
        copy.start()
        crossings.append(copy)
    own_mix = remote(mix_ref, mix_out.at[place.z, core], share.at[0, 0], share.at[1, 0], place.other)
    own_mix.start()
    own_moe = remote(
        moe_ref.at[place.ep],
        moe_out.at[place.ep, core],
        cross_share.at[0, 0],
        cross_share.at[1, 0],
        place.other,
    )
    own_moe.start()
    handed = []

    def hand_over(offset):
        crossings[offset - 1].wait_recv()
        slot = moe_out.at[place.source(offset), core]
        copy = remote(
            slot, slot, cross_share.at[0, offset], cross_share.at[1, offset], place.other
        )
        copy.start()
        handed.append(copy)

    order = list(range(1, n_ep))
    for distance in range(1, n_z):
        gather.step(distance)
        count = -(-len(order) // (n_z - distance))
        for offset in order[:count]:
            hand_over(offset)
        order = order[count:]
    gather.finish()
    for copy in crossings:
        copy.wait_send()
    for condition, make in sharing:
        pl.when(condition)(lambda make=make: make().wait())
    for copy in [own_mix, own_moe] + handed:
        copy.wait()
    for copy in here:
        copy.wait()


def spread(n_z, n_ep, mix_rows, moe_rows):
    return pl.pallas_call(
        functools.partial(spread_kernel, n_z, n_ep),
        out_shape=(
            jax.ShapeDtypeStruct((n_z, CORES) + mix_rows.shape, mix_rows.dtype),
            jax.ShapeDtypeStruct((n_ep, CORES) + moe_rows.shape[1:], moe_rows.dtype),
        ),
        in_specs=[VMEM, VMEM],
        out_specs=(ANY, ANY),
        scratch_shapes=[
            DMA((2, 2, n_z, 2)),
            DMA((2, 4 * n_z)),
            DMA((2, n_ep)),
            DMA((2, n_ep)),
            DMA((2,)),
        ],
        compiler_params=pltpu.CompilerParams(collective_id=1, has_side_effects=True),
        name="spread",
    )(mix_rows, moe_rows)


def add_into(target, terms):
    rows = target.shape[0]
    tall = 16 if rows % 16 == 0 else 8

    @pl.loop(0, rows // tall)
    def _(index):
        span = pl.ds(pl.multiple_of(index * tall, tall), tall)
        total = terms[0][span, :].astype(jnp.float32)
        for term in terms[1:]:
            total = total + term[span, :].astype(jnp.float32)
        target[span, :] = total.astype(target.dtype)


class LineReduce:
    def __init__(self, place, terms, total, landing, send, receive):
        self.place, self.terms, self.total, self.landing = place, terms, total, landing
        self.send, self.receive = send, receive
        self.pending = []

    def hop(self, way, z):
        where = self.place.up if way == 0 else self.place.down
        return remote(
            self.total.at[z],
            self.landing.at[way, z],
            self.send.at[z],
            self.receive.at[way, z],
            where,
        )

    def relay(self, way, z):
        place = self.place
        if way == 0:
            active, fed = place.z < z, place.has_down
        else:
            active, fed = place.z > z, place.has_up

        @pl.when(active & fed)
        def _():
            self.hop(way, z).wait_recv()
            add_into(self.total.at[z], self.terms(z) + [self.landing.at[way, z]])

        @pl.when(active & jnp.logical_not(fed))
        def _():
            add_into(self.total.at[z], self.terms(z))

        pl.when(active)(lambda: self.hop(way, z).start())
        self.pending.append((active, way, z))

    def step(self, number, prepare=None):
        for way, z in ((0, self.place.n_z - 1 - number), (1, number)):
            if prepare is not None:
                prepare(z)
            self.relay(way, z)

    def finish(self, out):
        place = self.place
        for z in range(place.n_z):
            landing = [self.landing.at[0, z], self.landing.at[1, z]]
            low, high = z > 0, z < place.n_z - 1

            @pl.when(place.z == z)
            def _(z=z, landing=landing, low=low, high=high):
                terms = self.terms(z)
                if low:
                    self.hop(0, z).wait_recv()
                    terms = terms + [landing[0]]
                if high:
                    self.hop(1, z).wait_recv()
                    terms = terms + [landing[1]]
                add_into(out, terms)

        for active, way, z in self.pending:
            pl.when(active)(lambda way=way, z=z: self.hop(way, z).wait_send())


def collect_kernel(
    n_z,
    n_ep,
    mix_ref,
    moe_ref,
    mix_out,
    moe_out,
    mix_own,
    mix_sib,
    mix_total,
    landing,
    moe_own,
    moe_sib,
    moe_total,
    line_send,
    line_receive,
    load_mix,
    load_moe,
    swap_mix,
    swap_moe,
    cross,
    local,
):
    place = Place(n_z, n_ep)
    core = place.core
    order = []
    for number in range(n_z):
        for z in (n_z - 1 - number, number):
            if z not in order:
                order.append(z)
    mix_loads, moe_loads = {}, []
    for z in order:
        mix_loads[z] = pltpu.make_async_copy(mix_ref.at[z, core], mix_own.at[z], load_mix.at[z])
        mix_loads[z].start()
    offsets = list(range(1, n_ep)) + [0]
    for offset in offsets:
        block = lax.rem(place.ep + offset, n_ep)
        copy = pltpu.make_async_copy(
            moe_ref.at[block, core], moe_own.at[offset], load_moe.at[offset]
        )
        copy.start()
        moe_loads.append(copy)
    greet(place, True, True, True)
    mix_swaps, moe_swaps = {}, []

    def swap(z):
        mix_swaps[z] = remote(
            mix_ref.at[z, 1 - core],
            mix_sib.at[z],
            swap_mix.at[0, z],
            swap_mix.at[1, z],
            place.other,
        )
        mix_swaps[z].start()

    for z in order[:2]:
        swap(z)
    for offset in offsets:
        block = lax.rem(place.ep + offset, n_ep)
        copy = remote(
            moe_ref.at[block, 1 - core],
            moe_sib.at[offset],
            swap_moe.at[0, offset],
            swap_moe.at[1, offset],
            place.other,
        )
        copy.start()
        moe_swaps.append(copy)
    for z in order[2:]:
        swap(z)

    ready = set()

    def prepare(z):
        if z not in ready:
            ready.add(z)
            mix_loads[z].wait()
            mix_swaps[z].wait_recv()

    chain = LineReduce(
        place,
        lambda z: [mix_own.at[z], mix_sib.at[z]],
        mix_total,
        landing,
        line_send,
        line_receive,
    )
    chain.step(0, prepare)
    crossings = []
    for index, offset in enumerate(offsets):
        moe_loads[index].wait()
        moe_swaps[index].wait_recv()
        add_into(moe_total.at[offset], [moe_own.at[offset], moe_sib.at[offset]])
        if offset:
            copy = remote(
                moe_total.at[offset],
                moe_out.at[place.ep],
                cross.at[0, offset],
                cross.at[1, offset],
                place.peer(offset),
            )
            copy.start()
            crossings.append(copy)
    kept = pltpu.make_async_copy(moe_total.at[0], moe_out.at[place.ep], local.at[0])
    kept.start()
    for number in range(1, n_z - 1):
        chain.step(number, prepare)
    for z in order:
        prepare(z)
    chain.finish(mix_out)
    for z in order:
        mix_swaps[z].wait_send()
    for copy in moe_swaps:
        copy.wait_send()
    for copy in crossings:
        copy.wait()
    kept.wait()


def collect(n_z, n_ep, mix_part, moe_part):
    mix_block, moe_block = mix_part.shape[2:], moe_part.shape[2:]
    bf16 = jnp.bfloat16
    return pl.pallas_call(
        functools.partial(collect_kernel, n_z, n_ep),
        out_shape=(
            jax.ShapeDtypeStruct(mix_block, bf16),
            jax.ShapeDtypeStruct((n_ep,) + moe_block, bf16),
        ),
        in_specs=[ANY, ANY],
        out_specs=(VMEM, ANY),
        scratch_shapes=[
            pltpu.VMEM((n_z,) + mix_block, bf16),
            pltpu.VMEM((n_z,) + mix_block, bf16),
            pltpu.VMEM((n_z,) + mix_block, bf16),
            pltpu.VMEM((2, n_z) + mix_block, bf16),
            pltpu.VMEM((n_ep,) + moe_block, bf16),
            pltpu.VMEM((n_ep,) + moe_block, bf16),
            pltpu.VMEM((n_ep,) + moe_block, bf16),
            DMA((n_z,)),
            DMA((2, n_z)),
            DMA((n_z,)),
            DMA((n_ep,)),
            DMA((2, n_z)),
            DMA((2, n_ep)),
            DMA((2, n_ep)),
            DMA((1,)),
        ],
        compiler_params=pltpu.CompilerParams(collective_id=2, has_side_effects=True),
        name="collect",
    )(mix_part, moe_part)


def token_reduce_kernel(n_z, n_ep, part_ref, out_ref, total, landing, send, receive):
    place = Place(n_z, n_ep)
    greet(place, True, False, False)
    chain = LineReduce(place, lambda z: [part_ref.at[z]], total, landing, send, receive)
    for number in range(n_z - 1):
        chain.step(number)
    chain.finish(out_ref)


def token_reduce(n_z, n_ep, part):
    block = part.shape[1:]
    return pl.pallas_call(
        functools.partial(token_reduce_kernel, n_z, n_ep),
        out_shape=jax.ShapeDtypeStruct(block, part.dtype),
        in_specs=[VMEM],
        out_specs=VMEM,
        scratch_shapes=[
            pltpu.VMEM((n_z,) + block, part.dtype),
            pltpu.VMEM((2, n_z) + block, part.dtype),
            DMA((n_z,)),
            DMA((2, n_z)),
        ],
        compiler_params=pltpu.CompilerParams(collective_id=3, has_side_effects=True),
        name="token_reduce",
    )(part)


def shards(
    mix_tokens,
    mix_gain,
    gate_proj,
    conv_proj,
    value_proj,
    conv_taps,
    out_proj,
    moe_tokens,
    moe_gain,
    expert_ids,
    expert_scores,
    expert_gate,
    expert_up,
    expert_down,
):
    n_ep, n_z = lax.axis_size("ep"), lax.axis_size("tp") // CORES
    width_model = moe_tokens.shape[1]
    moe_normed = scaled_norm(moe_tokens, moe_gain)
    experts = expert_gate.shape[0] * n_ep
    row_count, top_count = expert_ids.shape
    capacity = top_count * row_count // experts + max(1, top_count * row_count // (8 * experts))
    slots = n_z * capacity
    flat_ids = expert_ids.reshape(-1)
    onehot = (flat_ids[:, None] == jnp.arange(experts, dtype=jnp.int32)[None, :]).astype(jnp.int32)
    slot_rank = jnp.sum((jnp.cumsum(onehot, axis=0) - onehot) * onehot, axis=1)
    slot_index = flat_ids * slots + (lax.axis_index("tp") // CORES) * capacity + slot_rank
    route_weight = jax.nn.softmax(expert_scores, axis=1)
    meta = jnp.concatenate(
        [slot_index.reshape(row_count, top_count).T.astype(jnp.float32), route_weight.T], axis=0
    )
    lanes = -(-row_count // 128) * 128
    meta = jnp.pad(meta, ((0, -(-2 * top_count // 8) * 8 - 2 * top_count), (0, lanes - row_count)))
    gathered, meta_all = token_gather(n_z, n_ep, moe_normed, meta)
    targets = [
        meta_all[:, k, :row_count].reshape(-1).astype(jnp.int32) for k in range(top_count)
    ]
    weights = [meta_all[:, top_count + k, :row_count].reshape(-1) for k in range(top_count)]
    numbers = jnp.arange(experts * slots, dtype=jnp.int32)
    chosen = sum((numbers[:, None] == target[None, :]).astype(jnp.bfloat16) for target in targets)
    outgoing = jnp.dot(
        chosen, gathered.reshape(-1, width_model), preferred_element_type=jnp.float32
    ).astype(jnp.bfloat16)
    normed = scaled_norm(mix_tokens, mix_gain)
    mix_rows, moe_rows = spread(
        n_z, n_ep, normed, outgoing.reshape(experts, slots, width_model)
    )

    w_joint = jnp.concatenate([gate_proj, conv_proj, value_proj], axis=1)
    combined = jnp.dot(
        mix_rows.reshape(-1, width_model), w_joint, preferred_element_type=jnp.float32
    ).astype(jnp.bfloat16)
    channels = gate_proj.shape[1]
    out_gate = combined[:, :channels]
    in_gate = combined[:, channels : 2 * channels]
    values = combined[:, 2 * channels :]
    signal = (in_gate.astype(jnp.float32) * values.astype(jnp.float32)).astype(jnp.bfloat16)
    tap_count = conv_taps.shape[0]
    before = from_behind(signal[signal.shape[0] - (tap_count - 1) :], "ep", 1)
    portion = moe_rows.reshape(-1, width_model)
    gate_value = jnp.dot(portion, expert_gate[0], preferred_element_type=jnp.float32)
    up_value = jnp.dot(portion, expert_up[0], preferred_element_type=jnp.float32)
    hidden = (jax.nn.silu(gate_value) * up_value).astype(jnp.bfloat16)
    moe_part = jnp.dot(hidden, expert_down[0], preferred_element_type=jnp.float32).astype(
        jnp.bfloat16
    )
    extended = jnp.concatenate([before, signal], axis=0)
    length = signal.shape[0]
    tap_values = conv_taps.astype(jnp.float32)
    convolved = jnp.zeros((length, channels), jnp.float32)
    for offset in range(tap_count):
        convolved = (
            convolved + extended[offset : offset + length].astype(jnp.float32) * tap_values[offset]
        )
    carried = (out_gate.astype(jnp.float32) * convolved).astype(jnp.bfloat16)
    mix_part = jnp.dot(carried, out_proj, preferred_element_type=jnp.float32).astype(jnp.bfloat16)
    mix_out, returned = collect(
        n_z, n_ep, mix_part.reshape(mix_rows.shape), moe_part.reshape(moe_rows.shape)
    )
    mixing = sum(
        jnp.where(target[:, None] == numbers[None, :], weight[:, None], 0.0)
        for target, weight in zip(targets, weights)
    ).astype(jnp.bfloat16)
    moe_part = jnp.dot(
        mixing, returned.reshape(-1, width_model), preferred_element_type=jnp.float32
    ).astype(jnp.bfloat16)
    moe_out = token_reduce(n_z, n_ep, moe_part.reshape(n_z, row_count, width_model))
    return (mix_out, moe_out)


def solution(mesh):
    in_specs = (
        P(("ep", "tp"), None),
        P(),
        P(None, "tp"),
        P(None, "tp"),
        P(None, "tp"),
        P(None, "tp"),
        P("tp", None),
        P(("ep", "tp"), None),
        P(),
        P(("ep", "tp"), None),
        P(("ep", "tp"), None),
        P("ep", None, "tp"),
        P("ep", None, "tp"),
        P("ep", "tp", None),
    )
    out_specs = (P(("ep", "tp"), None), P(("ep", "tp"), None))
    return jax.shard_map(shards, mesh=mesh, in_specs=in_specs, out_specs=out_specs, check_vma=False)
```

```python
import functools
import jax
import jax.numpy as jnp
from jax import lax
from jax.experimental import pallas as pl
from jax.experimental.pallas import tpu as pltpu
from jax.sharding import PartitionSpec as P

norm_eps = 1e-06
CORES = 2
ANY = pl.BlockSpec(memory_space=pl.ANY)
VMEM = pl.BlockSpec(memory_space=pltpu.VMEM)
MESH = pl.DeviceIdType.MESH
DMA = pltpu.SemaphoreType.DMA


def from_behind(value, axis, steps):
    count = lax.axis_size(axis)
    leading, last = (max(0, -steps), min(count, count - steps))
    return lax.ppermute(value, axis, [(source, source + steps) for source in range(leading, last)])


def scaled_norm(row_data, gain_vec):
    values = row_data.astype(jnp.float32)
    inverse = lax.rsqrt(jnp.mean(values * values, axis=1, keepdims=True) + norm_eps)
    return (values * inverse * gain_vec.astype(jnp.float32)).astype(jnp.bfloat16)


class Place:
    def __init__(self, n_z, n_ep):
        self.n_z, self.n_ep = n_z, n_ep
        tp = lax.axis_index("tp")
        self.z, self.core = tp // CORES, lax.rem(tp, CORES)
        self.ep = lax.axis_index("ep")
        self.up = {"tp": lax.rem(tp + CORES, n_z * CORES)}
        self.down = {"tp": lax.rem(tp + (n_z - 1) * CORES, n_z * CORES)}
        self.other = {"tp": self.z * CORES + 1 - self.core}
        self.has_up, self.has_down = self.z < n_z - 1, self.z > 0

    def peer(self, offset):
        return {"ep": lax.rem(self.ep + offset, self.n_ep)}

    def source(self, offset):
        return lax.rem(self.ep + self.n_ep - offset, self.n_ep)


def greet(place, line, sibling, peers):
    barrier = pltpu.get_barrier_semaphore()

    def tell(where):
        pl.semaphore_signal(barrier, inc=1, device_id=where, device_id_type=MESH)

    if line:
        pl.when(place.has_up)(lambda: tell(place.up))
        pl.when(place.has_down)(lambda: tell(place.down))
    if sibling:
        tell(place.other)
    if peers:
        for offset in range(1, place.n_ep):
            tell(place.peer(offset))
    count = int(sibling) + (place.n_ep - 1 if peers else 0)
    if line:
        count = count + place.has_up.astype(jnp.int32) + place.has_down.astype(jnp.int32)
    pl.semaphore_wait(barrier, count)


def remote(source, target, send, receive, where):
    return pltpu.make_async_remote_copy(
        src_ref=source,
        dst_ref=target,
        send_sem=send,
        recv_sem=receive,
        device_id=where,
        device_id_type=MESH,
    )


class LineGather:
    def __init__(self, place, own, slot, parts, send, receive, on_arrival=None):
        self.place, self.own, self.slot, self.parts = place, own, slot, parts
        self.send, self.receive, self.on_arrival = send, receive, on_arrival
        self.pending = []

    def hop(self, way, step, part, source, z):
        where = self.place.up if way == 0 else self.place.down
        return remote(
            source,
            self.slot(z, part),
            self.send.at[way, step, part],
            self.receive.at[way, step, part],
            where,
        )

    def go(self, condition, make):
        pl.when(condition)(lambda: make().start())
        self.pending.append((condition, make))

    def begin(self):
        place = self.place
        for part in range(self.parts):
            for way, has in ((0, place.has_up), (1, place.has_down)):
                self.go(
                    has,
                    functools.partial(self.hop, way, 0, part, self.own(part), place.z),
                )

    def step(self, distance):
        place = self.place
        for part in range(self.parts):
            for way in (0, 1):
                if way == 0:
                    z, here, has = place.z - distance, place.z >= distance, place.has_up
                else:
                    z = place.z + distance
                    here, has = z < place.n_z, place.has_down
                z = lax.rem(z + place.n_z, place.n_z)
                incoming = functools.partial(
                    self.hop, way, distance - 1, part, self.own(part), z
                )
                pl.when(here)(lambda incoming=incoming: incoming().wait_recv())
                if distance < place.n_z - 1:
                    self.go(
                        here & has,
                        functools.partial(self.hop, way, distance, part, self.slot(z, part), z),
                    )
                if self.on_arrival is not None:
                    self.on_arrival(here, way, distance, part, z)

    def finish(self):
        for condition, make in self.pending:
            pl.when(condition)(lambda make=make: make().wait_send())


def token_gather_kernel(n_z, n_ep, rows_ref, meta_ref, rows_out, meta_out, sems, meta_sems, local):
    place = Place(n_z, n_ep)
    rows_here = pltpu.make_async_copy(rows_ref, rows_out.at[place.z], local.at[0])
    meta_here = pltpu.make_async_copy(meta_ref, meta_out.at[place.z], local.at[1])
    rows_here.start()
    meta_here.start()
    greet(place, True, False, False)
    half = rows_ref.shape[0] // 2
    gathers = [
        LineGather(
            place,
            lambda part: rows_ref.at[pl.ds(part * half, half)],
            lambda z, part: rows_out.at[z, pl.ds(part * half, half)],
            2,
            sems.at[0],
            sems.at[1],
        ),
        LineGather(
            place,
            lambda part: meta_ref,
            lambda z, part: meta_out.at[z],
            1,
            meta_sems.at[0],
            meta_sems.at[1],
        ),
    ]
    for gather in gathers:
        gather.begin()
    for distance in range(1, n_z):
        for gather in gathers:
            gather.step(distance)
    for gather in gathers:
        gather.finish()
    rows_here.wait()
    meta_here.wait()


def token_gather(n_z, n_ep, rows, meta):
    return pl.pallas_call(
        functools.partial(token_gather_kernel, n_z, n_ep),
        out_shape=(
            jax.ShapeDtypeStruct((n_z,) + rows.shape, rows.dtype),
            jax.ShapeDtypeStruct((n_z,) + meta.shape, meta.dtype),
        ),
        in_specs=[VMEM, VMEM],
        out_specs=(ANY, ANY),
        scratch_shapes=[DMA((2, 2, n_z, 2)), DMA((2, 2, n_z, 1)), DMA((2,))],
        compiler_params=pltpu.CompilerParams(collective_id=0, has_side_effects=True),
        name="token_gather",
    )(rows, meta)


def spread_kernel(
    n_z, n_ep, mix_ref, moe_ref, mix_out, moe_out, sems, share, cross, cross_share, local
):
    place = Place(n_z, n_ep)
    half = mix_ref.shape[0] // 2
    core = place.core
    sharing = []

    def mix_slot(z, part, which):
        return mix_out.at[z, which, pl.ds(part * half, half)]

    def share_copy(slot_here, slot_sem):
        return remote(
            slot_here, slot_here, share.at[0].at[slot_sem], share.at[1].at[slot_sem], place.other
        )

    here = [
        pltpu.make_async_copy(mix_ref, mix_out.at[place.z, core], local.at[0]),
        pltpu.make_async_copy(moe_ref.at[place.ep], moe_out.at[place.ep, core], local.at[1]),
    ]
    for copy in here:
        copy.start()
    greet(place, True, True, True)

    def on_arrival(condition, way, distance, part, z):
        sem = (way * n_z + distance) * 2 + part

        def make():
            return share_copy(mix_slot(z, part, core), sem)

        pl.when(condition)(lambda: make().start())
        sharing.append((condition, make))

    gather = LineGather(
        place,
        lambda part: mix_ref.at[pl.ds(part * half, half)],
        lambda z, part: mix_slot(z, part, core),
        2,
        sems.at[0],
        sems.at[1],
        on_arrival,
    )
    gather.begin()
    crossings = []
    for offset in range(1, n_ep):
        peer = place.peer(offset)
        copy = remote(
            moe_ref.at[peer["ep"]],
            moe_out.at[place.ep, core],
            cross.at[0, offset],
            cross.at[1, offset],
            peer,
        )
        copy.start()
        crossings.append(copy)
    own_mix = remote(mix_ref, mix_out.at[place.z, core], share.at[0, 0], share.at[1, 0], place.other)
    own_mix.start()
    own_moe = remote(
        moe_ref.at[place.ep],
        moe_out.at[place.ep, core],
        cross_share.at[0, 0],
        cross_share.at[1, 0],
        place.other,
    )
    own_moe.start()
    handed = []

    def hand_over(offset):
        crossings[offset - 1].wait_recv()
        slot = moe_out.at[place.source(offset), core]
        copy = remote(
            slot, slot, cross_share.at[0, offset], cross_share.at[1, offset], place.other
        )
        copy.start()
        handed.append(copy)

    order = list(range(1, n_ep))
    for distance in range(1, n_z):
        gather.step(distance)
        count = -(-len(order) // (n_z - distance))
        for offset in order[:count]:
            hand_over(offset)
        order = order[count:]
    gather.finish()
    for copy in crossings:
        copy.wait_send()
    for condition, make in sharing:
        pl.when(condition)(lambda make=make: make().wait())
    for copy in [own_mix, own_moe] + handed:
        copy.wait()
    for copy in here:
        copy.wait()


def spread(n_z, n_ep, mix_rows, moe_rows):
    return pl.pallas_call(
        functools.partial(spread_kernel, n_z, n_ep),
        out_shape=(
            jax.ShapeDtypeStruct((n_z, CORES) + mix_rows.shape, mix_rows.dtype),
            jax.ShapeDtypeStruct((n_ep, CORES) + moe_rows.shape[1:], moe_rows.dtype),
        ),
        in_specs=[VMEM, VMEM],
        out_specs=(ANY, ANY),
        scratch_shapes=[
            DMA((2, 2, n_z, 2)),
            DMA((2, 4 * n_z)),
            DMA((2, n_ep)),
            DMA((2, n_ep)),
            DMA((2,)),
        ],
        compiler_params=pltpu.CompilerParams(collective_id=1, has_side_effects=True),
        name="spread",
    )(mix_rows, moe_rows)


def add_into(target, terms):
    rows = target.shape[0]
    tall = 16 if rows % 16 == 0 else 8

    @pl.loop(0, rows // tall)
    def _(index):
        span = pl.ds(pl.multiple_of(index * tall, tall), tall)
        total = terms[0][span, :].astype(jnp.float32)
        for term in terms[1:]:
            total = total + term[span, :].astype(jnp.float32)
        target[span, :] = total.astype(target.dtype)


class LineReduce:
    def __init__(self, place, terms, total, landing, send, receive, parts=2):
        self.place, self.terms, self.total, self.landing = place, terms, total, landing
        self.send, self.receive, self.parts = send, receive, parts
        self.half = total.shape[1] // parts
        self.pending = []

    def span(self, ref, part):
        return ref.at[pl.ds(part * self.half, self.half)]

    def hop(self, way, z, part):
        where = self.place.up if way == 0 else self.place.down
        return remote(
            self.span(self.total.at[z], part),
            self.span(self.landing.at[way, z], part),
            self.send.at[z, part],
            self.receive.at[way, z, part],
            where,
        )

    def sums(self, z, part, landed=()):
        add_into(
            self.span(self.total.at[z], part),
            [self.span(term, part) for term in self.terms(z)] + list(landed),
        )

    def lead(self, number, prepare):
        place = self.place
        ends = ((0, place.n_z - 1 - number, place.z == 0), (1, number, place.z == place.n_z - 1))
        for way, z, end in ends:
            prepare(z)
        for way, z, end in ends:
            for part in range(self.parts):

                @pl.when(end)
                def _(way=way, z=z, part=part):
                    self.sums(z, part)
                    self.hop(way, z, part).start()

                self.pending.append((end, way, z, part))

    def relay(self):
        place, parts = self.place, self.parts
        for tick in range(1, (place.n_z - 1) * parts):
            for way in (0, 1):
                inner = place.z if way == 0 else place.n_z - 1 - place.z
                number = tick - inner
                beyond = (place.n_z - 1 - inner) * parts
                active = (inner > 0) & (number >= 0) & (number < beyond)
                safe = lax.rem(number + place.n_z * parts, place.n_z * parts)
                owner, part = safe // parts, lax.rem(safe, parts)
                z = place.n_z - 1 - owner if way == 0 else owner

                @pl.when(active)
                def _(way=way, z=z, part=part):
                    hop = self.hop(way, z, part)
                    hop.wait_recv()
                    self.sums(z, part, [self.span(self.landing.at[way, z], part)])
                    hop.start()

                self.pending.append((active, way, z, part))

    def finish(self, out):
        place = self.place
        for part in range(self.parts):
            for z in range(place.n_z):

                @pl.when(place.z == z)
                def _(z=z, part=part):
                    terms = [self.span(term, part) for term in self.terms(z)]
                    for way, fed in ((0, z > 0), (1, z < place.n_z - 1)):
                        if fed:
                            self.hop(way, z, part).wait_recv()
                            terms.append(self.span(self.landing.at[way, z], part))
                    add_into(self.span(out, part), terms)

        for active, way, z, part in self.pending:
            pl.when(active)(
                lambda way=way, z=z, part=part: self.hop(way, z, part).wait_send()
            )


def collect_kernel(
    n_z,
    n_ep,
    mix_ref,
    moe_ref,
    mixing_ref,
    mix_out,
    tokens_out,
    mix_own,
    mix_sib,
    mix_total,
    landing,
    moe_own,
    moe_sib,
    moe_total,
    arrived,
    tokens_own,
    tokens_total,
    tokens_landing,
    line_send,
    line_receive,
    tokens_send,
    tokens_receive,
    load_mix,
    load_moe,
    swap_mix,
    swap_moe,
    cross,
):
    place = Place(n_z, n_ep)
    core = place.core
    order = []
    for number in range(n_z):
        for z in (n_z - 1 - number, number):
            if z not in order:
                order.append(z)
    mix_loads, moe_loads = {}, []
    for z in order:
        mix_loads[z] = pltpu.make_async_copy(mix_ref.at[z, core], mix_own.at[z], load_mix.at[z])
        mix_loads[z].start()
    offsets = list(range(1, n_ep)) + [0]
    for offset in offsets:
        block = lax.rem(place.ep + offset, n_ep)
        copy = pltpu.make_async_copy(
            moe_ref.at[block, core], moe_own.at[offset], load_moe.at[offset]
        )
        copy.start()
        moe_loads.append(copy)
    greet(place, True, True, True)
    mix_swaps, moe_swaps = {}, []

    def swap(z):
        mix_swaps[z] = remote(
            mix_ref.at[z, 1 - core],
            mix_sib.at[z],
            swap_mix.at[0, z],
            swap_mix.at[1, z],
            place.other,
        )
        mix_swaps[z].start()

    def swap_rows(offset):
        block = lax.rem(place.ep + offset, n_ep)
        copy = remote(
            moe_ref.at[block, 1 - core],
            moe_sib.at[offset],
            swap_moe.at[0, offset],
            swap_moe.at[1, offset],
            place.other,
        )
        copy.start()
        moe_swaps.append(copy)

    for z in order[:2]:
        swap(z)
    swap_rows(offsets[0])
    for z in order[2:]:
        swap(z)
    for offset in offsets[1:]:
        swap_rows(offset)

    ready = set()

    def prepare(z):
        if z not in ready:
            ready.add(z)
            mix_loads[z].wait()
            mix_swaps[z].wait_recv()

    chain = LineReduce(
        place,
        lambda z: [mix_own.at[z], mix_sib.at[z]],
        mix_total,
        landing,
        line_send,
        line_receive,
    )
    chain.lead(0, prepare)
    crossings = []

    def cross_over(index):
        offset = offsets[index]
        moe_loads[index].wait()
        moe_swaps[index].wait_recv()
        target = moe_total.at[offset] if offset else arrived.at[place.ep]
        add_into(target, [moe_own.at[offset], moe_sib.at[offset]])
        if offset:
            copy = remote(
                moe_total.at[offset],
                arrived.at[place.ep],
                cross.at[0, offset],
                cross.at[1, offset],
                place.peer(offset),
            )
            copy.start()
            crossings.append(copy)

    cross_over(0)
    for number in range(1, n_z - 1):
        chain.lead(number, prepare)
    for index in range(1, n_ep):
        cross_over(index)
    chain.relay()
    for copy in crossings:
        copy.wait_recv()
    combine(n_z, n_ep, mixing_ref, arrived, tokens_own)
    tokens_chain = LineReduce(
        place,
        lambda z: [tokens_own.at[z]],
        tokens_total,
        tokens_landing,
        tokens_send,
        tokens_receive,
    )
    for number in range(n_z - 1):
        tokens_chain.lead(number, lambda z: None)
    for z in order:
        prepare(z)
    chain.finish(mix_out)
    tokens_chain.relay()
    tokens_chain.finish(tokens_out)
    for z in order:
        mix_swaps[z].wait_send()
    for copy in moe_swaps + crossings:
        copy.wait_send()


def combine(n_z, n_ep, mixing_ref, arrived, tokens_own):
    rows, width = tokens_own.shape[1], tokens_own.shape[2]
    tile = 256 if width % 256 == 0 else width

    @pl.loop(0, width // tile)
    def _(index):
        columns = pl.ds(pl.multiple_of(index * tile, tile), tile)
        total = jnp.zeros((n_z * rows, tile), jnp.float32)
        for expert in range(n_ep):
            total = total + jnp.dot(
                mixing_ref[expert],
                arrived[expert, :, columns],
                preferred_element_type=jnp.float32,
            )
        total = total.astype(tokens_own.dtype)
        for z in range(n_z):
            tokens_own[z, :, columns] = total[z * rows : (z + 1) * rows]


def collect(n_z, n_ep, mix_part, moe_part, mixing):
    mix_block, moe_block = mix_part.shape[2:], moe_part.shape[2:]
    tokens_block = (mixing.shape[1] // n_z, moe_block[1])
    bf16 = jnp.bfloat16
    return pl.pallas_call(
        functools.partial(collect_kernel, n_z, n_ep),
        out_shape=(
            jax.ShapeDtypeStruct(mix_block, bf16),
            jax.ShapeDtypeStruct(tokens_block, bf16),
        ),
        in_specs=[ANY, ANY, VMEM],
        out_specs=(VMEM, VMEM),
        scratch_shapes=[
            pltpu.VMEM((n_z,) + mix_block, bf16),
            pltpu.VMEM((n_z,) + mix_block, bf16),
            pltpu.VMEM((n_z,) + mix_block, bf16),
            pltpu.VMEM((2, n_z) + mix_block, bf16),
            pltpu.VMEM((n_ep,) + moe_block, bf16),
            pltpu.VMEM((n_ep,) + moe_block, bf16),
            pltpu.VMEM((n_ep,) + moe_block, bf16),
            pltpu.VMEM((n_ep,) + moe_block, bf16),
            pltpu.VMEM((n_z,) + tokens_block, bf16),
            pltpu.VMEM((n_z,) + tokens_block, bf16),
            pltpu.VMEM((2, n_z) + tokens_block, bf16),
            DMA((n_z, 2)),
            DMA((2, n_z, 2)),
            DMA((n_z, 2)),
            DMA((2, n_z, 2)),
            DMA((n_z,)),
            DMA((n_ep,)),
            DMA((2, n_z)),
            DMA((2, n_ep)),
            DMA((2, n_ep)),
        ],
        compiler_params=pltpu.CompilerParams(collective_id=2, has_side_effects=True),
        name="collect",
    )(mix_part, moe_part, mixing)


def shards(
    mix_tokens,
    mix_gain,
    gate_proj,
    conv_proj,
    value_proj,
    conv_taps,
    out_proj,
    moe_tokens,
    moe_gain,
    expert_ids,
    expert_scores,
    expert_gate,
    expert_up,
    expert_down,
):
    n_ep, n_z = lax.axis_size("ep"), lax.axis_size("tp") // CORES
    width_model = moe_tokens.shape[1]
    moe_normed = scaled_norm(moe_tokens, moe_gain)
    experts = expert_gate.shape[0] * n_ep
    row_count, top_count = expert_ids.shape
    capacity = top_count * row_count // experts + max(1, top_count * row_count // (8 * experts))
    slots = n_z * capacity
    ids_across = expert_ids.T
    earlier = jnp.arange(row_count)[:, None] < jnp.arange(row_count)[None, :]
    same = sum(
        (expert_ids[:, k][:, None, None] == ids_across[None]).astype(jnp.float32)
        for k in range(top_count)
    )
    slot_rank = jnp.sum(jnp.where(earlier[:, None, :], same, 0.0), axis=0)
    chip = lax.axis_index("tp") // CORES
    slot_index = (ids_across * slots + chip * capacity).astype(jnp.float32) + slot_rank
    scores = [expert_scores[:, k][None, :] for k in range(top_count)]
    largest = functools.reduce(jnp.maximum, scores)
    raised = [jnp.exp(score - largest) for score in scores]
    total = sum(raised)
    meta = jnp.concatenate([slot_index] + [value / total for value in raised], axis=0)
    lanes = -(-row_count // 128) * 128
    meta = jnp.pad(meta, ((0, -(-2 * top_count // 8) * 8 - 2 * top_count), (0, lanes - row_count)))
    gathered, meta_all = token_gather(n_z, n_ep, moe_normed, meta)
    targets = [
        meta_all[:, k, :row_count].reshape(-1).astype(jnp.int32) for k in range(top_count)
    ]
    weights = [meta_all[:, top_count + k, :row_count].reshape(-1) for k in range(top_count)]
    numbers = jnp.arange(experts * slots, dtype=jnp.int32)
    chosen = sum((numbers[:, None] == target[None, :]).astype(jnp.bfloat16) for target in targets)
    outgoing = jnp.dot(
        chosen, gathered.reshape(-1, width_model), preferred_element_type=jnp.float32
    ).astype(jnp.bfloat16)
    normed = scaled_norm(mix_tokens, mix_gain)
    mix_rows, moe_rows = spread(
        n_z, n_ep, normed, outgoing.reshape(experts, slots, width_model)
    )

    w_joint = jnp.concatenate([gate_proj, conv_proj, value_proj], axis=1)
    combined = jnp.dot(
        mix_rows.reshape(-1, width_model), w_joint, preferred_element_type=jnp.float32
    ).astype(jnp.bfloat16)
    channels = gate_proj.shape[1]
    out_gate = combined[:, :channels]
    in_gate = combined[:, channels : 2 * channels]
    values = combined[:, 2 * channels :]
    signal = (in_gate.astype(jnp.float32) * values.astype(jnp.float32)).astype(jnp.bfloat16)
    tap_count = conv_taps.shape[0]
    before = from_behind(signal[signal.shape[0] - (tap_count - 1) :], "ep", 1)
    portion = moe_rows.reshape(-1, width_model)
    gate_value = jnp.dot(portion, expert_gate[0], preferred_element_type=jnp.float32)
    up_value = jnp.dot(portion, expert_up[0], preferred_element_type=jnp.float32)
    hidden = lax.optimization_barrier(
        (jax.nn.silu(gate_value) * up_value).astype(jnp.bfloat16)
    )
    moe_part = jnp.dot(hidden, expert_down[0], preferred_element_type=jnp.float32).astype(
        jnp.bfloat16
    )
    extended = jnp.concatenate([before, signal], axis=0)
    length = signal.shape[0]
    tap_values = conv_taps.astype(jnp.float32)
    convolved = jnp.zeros((length, channels), jnp.float32)
    for offset in range(tap_count):
        convolved = (
            convolved + extended[offset : offset + length].astype(jnp.float32) * tap_values[offset]
        )
    carried = (out_gate.astype(jnp.float32) * convolved).astype(jnp.bfloat16)
    mix_part = jnp.dot(carried, out_proj, preferred_element_type=jnp.float32).astype(jnp.bfloat16)
    places = numbers.reshape(n_ep, 1, -1)
    mixing = sum(
        jnp.where(target[None, :, None] == places, weight[None, :, None], 0.0)
        for target, weight in zip(targets, weights)
    ).astype(jnp.bfloat16)
    mix_out, moe_out = collect(
        n_z, n_ep, mix_part.reshape(mix_rows.shape), moe_part.reshape(moe_rows.shape), mixing
    )
    return (mix_out, moe_out)


def solution(mesh):
    in_specs = (
        P(("ep", "tp"), None),
        P(),
        P(None, "tp"),
        P(None, "tp"),
        P(None, "tp"),
        P(None, "tp"),
        P("tp", None),
        P(("ep", "tp"), None),
        P(),
        P(("ep", "tp"), None),
        P(("ep", "tp"), None),
        P("ep", None, "tp"),
        P("ep", None, "tp"),
        P("ep", "tp", None),
    )
    out_specs = (P(("ep", "tp"), None), P(("ep", "tp"), None))
    return jax.shard_map(shards, mesh=mesh, in_specs=in_specs, out_specs=out_specs, check_vma=False)
```
